32 devices in a mesh: kv: 8 (over z, y), tp: 4 (over x, core).
Axes of the slice: x: 2, y: 2, z: 4, core: 2. Of those that a mesh axis runs over, the one named last changes fastest.
Arguments:
- tokens: bfloat16 [128, 4096], P(None, ('kv', 'tp')), may hold values from -64 to 64
- mix_gain: float32 [4096], P('kv'), may hold values from 0.1 to 1.9
- w_query: bfloat16 [4096, 3072], P('kv', 'tp'), may hold values from -0.09375 to 0.09375
- w_key: bfloat16 [4096, 3072], P('kv', 'tp'), may hold values from -0.09375 to 0.09375
- w_value: bfloat16 [4096, 3072], P('kv', 'tp'), may hold values from -0.09375 to 0.09375
- w_gate: bfloat16 [4096, 3072], P('kv', 'tp'), may hold values from -0.09375 to 0.09375
- w_beta: bfloat16 [4096, 24], P('kv'), may hold values from -0.09375 to 0.09375
- w_decay: bfloat16 [4096, 24], P('kv'), may hold values from -0.09375 to 0.09375
- decay_rate: float32 [24], P('tp'), may hold values from 0.15 to 1.5
- out_gain: float32 [128], replicated, may hold values from 0.1 to 1.9
- state: float32 [128, 24, 128, 128], P('kv', 'tp'), may hold values from -0.6 to 0.6
- w_out: bfloat16 [3072, 4096], P('tp', 'kv'), may hold values from -0.109375 to 0.109375
- mlp_gain: float32 [4096], replicated, may hold values from 0.1 to 1.9
- w_up: bfloat16 [4096, 16384], P(None, ('kv', 'tp')), may hold values from -0.09375 to 0.09375
- w_down: bfloat16 [16384, 4096], P(('kv', 'tp')), may hold values from -0.09375 to 0.09375
Outputs:
- mixed: bfloat16 [128, 4096], P(None, ('kv', 'tp'))
- new_state: float32 [128, 24, 128, 128], P('kv', 'tp')
The draws below stay inside these ranges and needn't reach their ends.
All inputs are finite; a program needn't handle non-finite values.
Results may differ from the reference program's by a relative error of at most 0.0063.
Values may be sent and summed in bfloat16 or wider, within the bound.
No kernel may reach another device: no remote copies, remote signals or barrier semaphores. Data moves between devices by JAX's collectives and lax.ppermute only.
A program may use at most 64 MiB of HBM per device.

```python
import math
import jax
import jax.numpy as jnp
from jax import lax

D = 4096
H = 24
HEAD = 128
FF = 16384
BATCH = 128


def draw_tokens(key, part):
    first, second, third = jax.random.split(jax.random.fold_in(key, 17), 3)
    position = jnp.arange(D, dtype=jnp.float32) / D
    column_scale = jnp.exp(jnp.log(6.0) * (position - 0.5)) * jax.random.uniform(second, (D,), jnp.float32, 0.6, 1.6)
    base = jnp.clip(jax.random.normal(first, (BATCH, D), jnp.float32), -4.0, 4.0)
    row_scale = jnp.exp(jax.random.uniform(third, (BATCH, 1), jnp.float32, jnp.log(0.4), jnp.log(4.0)))
    values = base * row_scale * column_scale[None, :]
    return values.astype(jnp.bfloat16)


def raised(entries, rng, source, target, parts, factor):
    owner, partner = [(jnp.arange(entries.shape[dim]) // (entries.shape[dim] // parts)).reshape([-1 if axis == dim else 1 for axis in range(entries.ndim)]) for dim in (source, target)]
    chosen = jax.random.permutation(rng, parts)[partner]
    strong = (owner == chosen) | (owner == (partner + parts // 2) % parts)
    return jnp.where(strong, factor * entries, entries)


def levels(own_key, extent, cuts, least, top_value):
    def one(dim, parts):
        steps = jax.random.uniform(jax.random.fold_in(jax.random.fold_in(own_key, 6), dim), (parts,), jnp.float32, least / len(cuts), top_value / len(cuts))
        return jnp.repeat(jnp.exp(steps), extent[dim] // parts).reshape((-1,) + (1,) * (len(extent) - dim - 1))

    level = one(*cuts[0])
    for cut in cuts[1:]:
        level = level * one(*cut)
    return level


def noise(own_key, extent, deviation, bound, cuts=(), kind=jnp.bfloat16):
    values = deviation * jax.random.normal(own_key, extent, jnp.float32)
    if cuts:
        values = values * levels(own_key, extent, cuts, -0.22, 0.18)
    return jnp.clip(values, -bound, bound).astype(kind)


def gaussian_with(rng, dims, deviation, limit, pieces, heavy, kind=jnp.bfloat16):
    values = deviation * jax.random.normal(rng, dims, jnp.float32)
    if pieces:
        values = values * levels(rng, dims, pieces, -0.22, 0.18)
    return jnp.clip(raised(values, jax.random.fold_in(rng, 3), *heavy), -limit, limit).astype(kind)


def setup_inputs(seed: int = 0) -> dict:
    key_of = jax.random.split(jax.random.key(seed), 16)
    return {
        "tokens": draw_tokens(jax.random.fold_in(key_of[15], 71), 0),
        "mix_gain": jnp.clip(1.0 + 0.18 * jax.random.normal(key_of[1], (D,), jnp.float32), 0.1, 1.9),
        "w_query": noise(key_of[2], (D, H * HEAD), D ** -0.5, 0.09375, ((0, 8), (1, 4))),
        "w_key": noise(key_of[3], (D, H * HEAD), D ** -0.5, 0.09375, ((0, 8), (1, 4))),
        "w_value": noise(key_of[4], (D, H * HEAD), D ** -0.5, 0.09375, ((0, 8), (1, 4))),
        "w_gate": noise(key_of[5], (D, H * HEAD), D ** -0.5, 0.09375, ((0, 8), (1, 4))),
        "w_beta": noise(key_of[6], (D, H), D ** -0.5, 0.09375, ((0, 8),)),
        "w_decay": noise(key_of[7], (D, H), D ** -0.5, 0.09375, ((0, 8),)),
        "decay_rate": jnp.clip(jnp.exp(math.log(1.5) - 2.3025851 * jax.random.uniform(key_of[8], (H,), jnp.float32) ** levels(key_of[8], (H,), ((0, 4),), -0.2, 0.2)), 0.15, 1.5),
        "out_gain": jnp.clip(1.0 + 0.18 * jax.random.normal(key_of[9], (HEAD,), jnp.float32), 0.1, 1.9),
        "state": noise(key_of[10], (BATCH, H, HEAD, HEAD), 0.1, 0.6, ((0, 8), (1, 4)), jnp.float32),
        "w_out": noise(key_of[11], (H * HEAD, D), (H * HEAD) ** -0.5, 0.109375, ((0, 4), (1, 8))),
        "mlp_gain": jnp.clip(1.0 + 0.18 * jax.random.normal(key_of[12], (D,), jnp.float32), 0.1, 1.9),
        "w_up": noise(key_of[13], (D, FF), D ** -0.5, 0.09375, ((1, 32),)),
        "w_down": gaussian_with(key_of[14], (FF, D), FF ** -0.5, 0.09375, ((0, 32),), (0, 1, 32, 2.75)),
    }


EPSILON = 1e-06

def head_norm(values):
    return values * lax.rsqrt(lax.optimization_barrier(jnp.sum(values * values, axis=-1, keepdims=True)) + EPSILON)

def per_head(inputs):
    old_state, decay, key, value, beta, query = inputs
    faded = old_state * decay[:, None, None]
    recalled = jnp.einsum('bkv,bk->bv', faded, key, precision=lax.Precision.HIGHEST)
    change = beta[:, None] * (value - recalled)
    updated = faded + key[:, :, None] * change[:, None, :]
    readout = jnp.einsum('bkv,bk->bv', updated, query, precision=lax.Precision.HIGHEST)
    return (updated, readout)

def reference(tokens, mix_gain, w_query, w_key, w_value, w_gate, w_beta, w_decay, decay_rate, out_gain, state, w_out, mlp_gain, w_up, w_down):
    tokens_f = tokens.astype(jnp.float32)
    row_scale = lax.rsqrt(lax.optimization_barrier(jnp.mean(tokens_f * tokens_f, axis=1, keepdims=True)) + EPSILON)
    normed = (tokens_f * mix_gain[None, :]).astype(jnp.bfloat16)

    def project(weight):
        return jnp.dot(normed, weight, preferred_element_type=jnp.float32) * row_scale
    query_raw = project(w_query).reshape(BATCH, H, HEAD)
    key_raw = project(w_key).reshape(BATCH, H, HEAD)
    value_raw = project(w_value).reshape(BATCH, H, HEAD)
    gate_raw = project(w_gate).reshape(BATCH, H, HEAD)
    beta_raw = project(w_beta)
    decay_raw = project(w_decay)
    query = head_norm(jax.nn.silu(query_raw)) * HEAD ** (-0.5)
    key = head_norm(jax.nn.silu(key_raw))
    value = jax.nn.silu(value_raw)
    beta = jax.nn.sigmoid(beta_raw)
    decay = jnp.exp(-decay_rate[None, :] * jax.nn.softplus(decay_raw))
    updated, readout = lax.map(per_head, (jnp.moveaxis(state, 1, 0), decay.T, jnp.moveaxis(key, 1, 0), jnp.moveaxis(value, 1, 0), beta.T, jnp.moveaxis(query, 1, 0)))
    new_state = jnp.moveaxis(updated, 0, 1)
    readout = jnp.moveaxis(readout, 0, 1)
    scaled = readout * lax.rsqrt(lax.optimization_barrier(jnp.mean(readout * readout, axis=-1, keepdims=True)) + EPSILON) * out_gain
    merged = (scaled * jax.nn.silu(gate_raw)).reshape(BATCH, H * HEAD).astype(jnp.bfloat16)
    residual = (tokens_f + jnp.dot(merged, w_out, preferred_element_type=jnp.float32)).astype(jnp.bfloat16)
    residual_f = residual.astype(jnp.float32)
    normed_mlp = (residual_f * lax.rsqrt(lax.optimization_barrier(jnp.mean(residual_f * residual_f, axis=1, keepdims=True)) + EPSILON) * mlp_gain[None, :]).astype(jnp.bfloat16)
    hidden = jnp.square(jax.nn.relu(jnp.dot(normed_mlp, w_up, preferred_element_type=jnp.float32))).astype(jnp.bfloat16)
    mixed = (residual_f + jnp.dot(hidden, w_down, preferred_element_type=jnp.float32)).astype(jnp.bfloat16)
    return (mixed, new_state)
```

```python
import jax
import jax.numpy as jnp
from jax import lax
from jax.sharding import PartitionSpec as P

EPSILON = 1e-06
F32 = jnp.float32
BF16 = jnp.bfloat16


def split_axis(size):
    inner = 1
    for f in range(1, size + 1):
        if f * f <= size and size % f == 0:
            inner = f
    return size // inner, inner


class Ring:
    def __init__(self, axis, total, n, inner):
        self.axis, self.total, self.n, self.inner = axis, total, n, inner

    def coord(self):
        return (lax.axis_index(self.axis) // self.inner) % self.n

    def send(self, value, shift):
        pairs = []
        for i in range(self.total):
            c = (i // self.inner) % self.n
            pairs.append((i, i + ((c + shift) % self.n - c) * self.inner))
        return lax.ppermute(value, self.axis, pairs)


def gather(ring, x):
    n = ring.n
    if n == 1:
        return x[None]
    c = ring.coord()
    parts = [x] + [ring.send(x, s) for s in range(1, n)]
    if n == 2:
        first = c == 0
        return jnp.stack([jnp.where(first, parts[0], parts[1]), jnp.where(first, parts[1], parts[0])])
    back = jnp.stack(parts[::-1])
    return lax.dynamic_slice_in_dim(jnp.concatenate([back, back]), n - 1 - c, n, 0)


def pack(block, exact):
    if not exact:
        return block.astype(BF16)
    tail = block[..., -exact:]
    high = lax.reduce_precision(tail, 8, 7)
    low = (tail - high).astype(BF16)
    return jnp.concatenate([block[..., :-exact].astype(BF16), high.astype(BF16), low], axis=-1)


def unpack(block, exact):
    block = block.astype(F32)
    if not exact:
        return block
    tail = block[..., -2 * exact : -exact] + block[..., -exact:]
    return jnp.concatenate([block[..., : -2 * exact], tail], axis=-1)


def scatter_sum(ring, x, exact=0):
    n = ring.n
    c = ring.coord()
    received = [
        ring.send(pack(lax.dynamic_index_in_dim(x, (c + s) % n, 0, False), exact), s)
        for s in range(1, n)
    ]
    total = lax.dynamic_index_in_dim(x, c, 0, False)
    for r in received:
        total = total + unpack(r, exact)
    return total


def head_norm(values):
    return values * lax.rsqrt(jnp.sum(values * values, axis=-1, keepdims=True) + EPSILON)


def make_local(kv, tp):
    nz, ny = split_axis(kv)
    nc = 2 if tp % 2 == 0 else 1
    nx = tp // nc
    ring_z = Ring("kv", kv, nz, ny)
    ring_y = Ring("kv", kv, ny, 1)
    ring_x = Ring("tp", tp, nx, nc)
    ring_c = Ring("tp", tp, nc, 1)

    def local(
        tokens,
        mix_gain,
        w_query,
        w_key,
        w_value,
        w_gate,
        w_beta,
        w_decay,
        decay_rate,
        out_gain,
        state,
        w_out,
        mlp_gain,
        w_up,
        w_down,
    ):
        batch, own_columns = tokens.shape
        rows, heads, size = state.shape[0], state.shape[1], state.shape[2]
        wide = heads * size
        all_heads = w_beta.shape[1]
        d_model = w_up.shape[0]

        columns = gather(ring_c, gather(ring_x, tokens))
        columns = columns.transpose(2, 1, 0, 3).reshape(batch, tp * own_columns)
        columns_f = columns.astype(F32)
        normed = (columns_f * mix_gain[None, :]).astype(BF16)

        def project(weight):
            return jnp.dot(normed, weight, preferred_element_type=F32)

        squares = jnp.sum(columns_f * columns_f, axis=1, keepdims=True)
        rates_part = project(jnp.concatenate([w_beta, w_decay], axis=1))
        exact = 2 * all_heads + 1

        def over_y(pieces, exact):
            part = jnp.concatenate(pieces, axis=1)
            part = part.reshape(nz, ny, rows, part.shape[1]).swapaxes(0, 1)
            return scatter_sum(ring_y, part, exact)

        first = over_y([project(w_query), project(w_key)], 0)
        second = over_y([project(w_value), project(w_gate), rates_part, squares], exact)
        summed = scatter_sum(ring_z, jnp.concatenate([first, second], axis=-1), exact)

        row_scale = lax.rsqrt(summed[:, -1:] / d_model + EPSILON)
        shape_heads = (rows, heads, size)

        def raw(i):
            return (summed[:, i * wide : (i + 1) * wide] * row_scale).reshape(shape_heads)

        query = head_norm(jax.nn.silu(raw(0))) * size ** (-0.5)
        key = head_norm(jax.nn.silu(raw(1)))
        value = jax.nn.silu(raw(2))
        gate_raw = raw(3)
        rates = summed[:, 4 * wide : 4 * wide + 2 * all_heads] * row_scale
        head_start = lax.axis_index("tp") * heads
        beta = jax.nn.sigmoid(lax.dynamic_slice_in_dim(rates, head_start, heads, 1))
        decay_raw = lax.dynamic_slice_in_dim(rates, all_heads + head_start, heads, 1)
        decay = jnp.exp(-decay_rate[None, :] * jax.nn.softplus(decay_raw))[:, :, None]

        by_key = jnp.sum(state * key[:, :, :, None], axis=2)
        by_query = jnp.sum(state * query[:, :, :, None], axis=2)
        change = beta[:, :, None] * (value - decay * by_key)
        new_state = state * decay[..., None] + key[:, :, :, None] * change[:, :, None, :]
        readout = decay * by_query + jnp.sum(key * query, axis=-1, keepdims=True) * change
        scaled = (
            readout
            * lax.rsqrt(jnp.mean(readout * readout, axis=-1, keepdims=True) + EPSILON)
            * out_gain
        )
        merged = (scaled * jax.nn.silu(gate_raw)).reshape(rows, wide).astype(BF16)

        merged = gather(ring_y, gather(ring_z, merged))
        merged = merged.swapaxes(0, 1).reshape(batch, wide)
        partial_out = jnp.dot(merged, w_out, preferred_element_type=F32)
        partial_out = partial_out.reshape(batch, nx, nc, own_columns).transpose(2, 1, 0, 3)
        branch_sum = scatter_sum(ring_x, scatter_sum(ring_c, partial_out))
        residual = (tokens.astype(F32) + branch_sum).astype(BF16)

        whole = gather(ring_c, gather(ring_x, gather(ring_y, gather(ring_z, residual))))
        whole = whole.transpose(4, 3, 2, 1, 0, 5).reshape(batch, d_model)
        whole_f = whole.astype(F32)
        normed_mlp = (
            whole_f
            * lax.rsqrt(jnp.mean(whole_f * whole_f, axis=1, keepdims=True) + EPSILON)
            * mlp_gain[None, :]
        ).astype(BF16)
        hidden = jnp.square(
            jax.nn.relu(jnp.dot(normed_mlp, w_up, preferred_element_type=F32))
        ).astype(BF16)
        partial = jnp.dot(hidden, w_down, preferred_element_type=F32)
        partial = partial.reshape(batch, nz, ny, nx, nc, own_columns).transpose(4, 3, 2, 1, 0, 5)
        branch = scatter_sum(ring_c, partial)
        branch = scatter_sum(ring_x, branch)
        branch = scatter_sum(ring_y, branch)
        branch = scatter_sum(ring_z, branch)
        mixed = (residual.astype(F32) + branch).astype(BF16)
        return (mixed, new_state)

    return local


def solution(mesh):
    placed = (
        P(None, ("kv", "tp")),
        P("kv"),
        P("kv", "tp"),
        P("kv", "tp"),
        P("kv", "tp"),
        P("kv", "tp"),
        P("kv", None),
        P("kv", None),
        P("tp"),
        P(),
        P("kv", "tp", None, None),
        P("tp", "kv"),
        P(),
        P(None, ("kv", "tp")),
        P(("kv", "tp"), None),
    )
    return jax.shard_map(
        make_local(mesh.shape["kv"], mesh.shape["tp"]),
        mesh=mesh,
        in_specs=placed,
        out_specs=(P(None, ("kv", "tp")), P("kv", "tp", None, None)),
        check_vma=False,
    )
```
